32 devices in a mesh: tp: 8 (over z, x), dp: 4 (over y, core).
Axes of the slice: x: 2, y: 2, z: 4, core: 2. Of those that a mesh axis runs over, the one named last changes fastest.
Arguments:
- tokens: bfloat16 [128, 8, 4096], P('dp', None, 'tp'), may hold values from -12 to 12
- lengths: int32 [128], P('dp'), may hold values from 1 to 8, 384 in all
- norm_gains: float32 [2, 4096], replicated, may hold values from 0.1 to 1.9
- drive_proj: bfloat16 [2, 4096, 2048], P(None, 'dp', 'tp'), may hold values from -0.09375 to 0.09375
- open_proj: bfloat16 [2, 4096, 4096], P(None, 'dp', 'tp'), may hold values from -0.09375 to 0.09375
- glu_proj: bfloat16 [2, 2048, 2048], P(None, 'dp', 'tp'), may hold values from -0.125 to 0.125
- merge_proj: bfloat16 [2, 2048, 4096], P(None, 'dp', 'tp'), may hold values from -0.125 to 0.125
- exit_proj: bfloat16 [2, 4096, 4096], P(None, 'dp', 'tp'), may hold values from -0.09375 to 0.09375
- decay_rate: float32 [2, 128, 64], P(None, 'tp'), may hold values from 0.5 to 2
- turn_rate: float32 [2, 128, 64], P(None, 'tp'), may hold values from -3 to 3
- group_step_width: float32 [2, 128], P(None, 'tp'), may hold values from 0.005 to 0.3
- state_in: float32 [2, 2, 128, 64, 16], P(None, None, 'tp'), may hold values from -1 to 1
- state_out: float32 [2, 2, 128, 16, 64], P(None, None, 'tp'), may hold values from -0.5 to 0.5
- skip_gain: float32 [2, 2048], P(None, 'tp'), may hold values from -4 to 4
- carried_state: float32 [2, 2, 128, 8192], P(None, None, 'dp', 'tp'), may hold values from -6 to 6
Outputs:
- updated_tokens: bfloat16 [128, 8, 4096], P('dp', None, 'tp')
- new_state: float32 [2, 2, 128, 8192], P(None, None, 'dp', 'tp')
The draws below stay inside these ranges and needn't reach their ends.
Inputs may be any that keep to these rules, and one draw needn't show every extreme that they name: `lengths`: each sequence has at least one live slot, and some sequence has all 8.
All inputs are finite; a program needn't handle non-finite values. No bound on the sum of `lengths` on one device may be relied on, other than what follows from the above.
Results may differ from the reference program's by a relative error of at most 0.0055.
Values may be sent and summed in bfloat16 or wider, within the bound.
No kernel may reach another device: no remote copies, remote signals or barrier semaphores. Data moves between devices by JAX's collectives and lax.ppermute only.
A program may use at most 128 MiB of HBM per device.

```python
import math
import jax
import jax.numpy as jnp
import numpy as np
from jax import lax

D = 4096
WIDTH = 2048
CHANNELS = 16
STATE = 64
STEPS = 8
LAYERS = 2
GROUPS = 128
BATCH = 128


def draw_tokens(key, part):
    first_key, second_key = jax.random.split(jax.random.fold_in(key, 11))
    block_count = 32
    blocks = jax.random.uniform(second_key, (BATCH, 1, block_count, 1), jnp.float32, math.log(0.3), math.log(3.0))
    factor = jnp.exp(blocks)
    values_drawn = jnp.clip(jax.random.normal(first_key, (BATCH, STEPS, block_count, D // block_count), jnp.float32), -4.0, 4.0)
    return (values_drawn * factor).reshape(BATCH, STEPS, D).astype(jnp.bfloat16)


def levels(key, shape, cuts, low, top_value):
    def one(dim, shards_of):
        heights = jax.random.uniform(jax.random.fold_in(jax.random.fold_in(key, 6), dim), (shards_of,), jnp.float32, low / len(cuts), top_value / len(cuts))
        return jnp.repeat(jnp.exp(heights), shape[dim] // shards_of).reshape((-1,) + (1,) * (len(shape) - dim - 1))

    gain = one(*cuts[0])
    for cut in cuts[1:]:
        gain = gain * one(*cut)
    return gain


def split_up(number_of, total, limit, slope):
    loads = [(1 << 20) // math.isqrt(grade ** slope) + 1 for grade in range(2, number_of + 1)]
    surplus, holding = total - limit - (number_of - 1), [1] * (number_of - 1)
    while surplus > 0:
        movable = [i for i in range(number_of - 1) if holding[i] < limit]
        pool, left = sum([loads[i] for i in movable]), surplus
        for i in movable:
            more = min(limit - holding[i], max(1, left * loads[i] // pool), surplus)
            holding[i] = holding[i] + more
            surplus = surplus - more
    return np.array([limit] + holding)


def uneven(stream_key, amount, total, reach, lean):
    if amount == 2:
        one = jax.random.randint(stream_key, (), max(1, total - reach), min(reach, total - 1) + 1)
        return jnp.stack([one, total - one])
    sizes = jnp.asarray(split_up(amount, total, reach, lean), jnp.int32)
    twos = (amount - 1) // 2
    donor, sink = sizes[1:1 + 2 * twos:2], sizes[2:2 + 2 * twos:2]
    room = jnp.minimum(donor - 1, reach - sink)
    passed = jax.random.randint(jax.random.fold_in(stream_key, 1), (twos,), 0, 1 << 20) % (room + 1)
    sizes = sizes.at[1:1 + 2 * twos:2].set(donor - passed).at[2:2 + 2 * twos:2].set(sink + passed)
    return sizes[jax.random.permutation(jax.random.fold_in(stream_key, 2), amount)]


def gaussian(stream_key, extent, scale, limit, cuts=(), dtype=jnp.bfloat16):
    loudness = levels(stream_key, extent, cuts, -0.22, 0.18) if cuts else 1.0
    array = jax.random.normal(stream_key, extent, jnp.float32) * scale * loudness
    return jnp.minimum(jnp.maximum(array, -limit), limit).astype(dtype)


def setup_inputs(seed: int = 0) -> dict:
    splits = jax.random.split(jax.random.key(seed), 16)
    return {
        "tokens": draw_tokens(jax.random.fold_in(splits[15], 71), 0),
        "lengths": uneven(splits[1], BATCH, 3 * BATCH, STEPS, 2).astype(jnp.int32),
        "norm_gains": jnp.clip(1.0 + 0.18 * jax.random.normal(splits[2], (LAYERS, D), jnp.float32), 0.1, 1.9),
        "drive_proj": gaussian(splits[3], (LAYERS, D, WIDTH), D ** -0.5, 0.09375, ((1, 4), (2, 8))),
        "open_proj": gaussian(splits[4], (LAYERS, D, D), D ** -0.5, 0.09375, ((1, 4), (2, 8))),
        "glu_proj": gaussian(splits[5], (LAYERS, WIDTH, WIDTH), WIDTH ** -0.5, 0.125, ((1, 4), (2, 8))),
        "merge_proj": gaussian(splits[6], (LAYERS, WIDTH, D), WIDTH ** -0.5, 0.125, ((1, 4), (2, 8))),
        "exit_proj": gaussian(splits[7], (LAYERS, D, D), D ** -0.5, 0.09375, ((1, 4), (2, 8))),
        "decay_rate": jnp.clip(jnp.exp(math.log(2.0) - 1.3862944 * jax.random.uniform(splits[8], (LAYERS, GROUPS, STATE), jnp.float32) ** levels(splits[8], (LAYERS, GROUPS, STATE), ((1, 8),), -0.2, 0.2)), 0.5, 2.0),
        "turn_rate": jnp.clip(jax.random.uniform(splits[9], (LAYERS, GROUPS, STATE), jnp.float32, -3.0, 3.0) * levels(splits[9], (LAYERS, GROUPS, STATE), ((1, 8),), -0.4, 0.0), -3.0, 3.0),
        "group_step_width": jnp.clip(jnp.exp(math.log(0.3) - 4.0943446 * jax.random.uniform(splits[10], (LAYERS, GROUPS), jnp.float32) ** levels(splits[10], (LAYERS, GROUPS), ((1, 8),), -0.2, 0.2)), 0.005, 0.3),
        "state_in": gaussian(splits[11], (LAYERS, 2, GROUPS, STATE, CHANNELS), (2 * CHANNELS) ** -0.5, 1.0, ((2, 8),), jnp.float32),
        "state_out": gaussian(splits[12], (LAYERS, 2, GROUPS, CHANNELS, STATE), (2 * STATE) ** -0.5, 0.5, ((2, 8),), jnp.float32),
        "skip_gain": gaussian(splits[13], (LAYERS, WIDTH), 1.0, 4.0, ((1, 8),), jnp.float32),
        "carried_state": gaussian(splits[14], (LAYERS, 2, BATCH, GROUPS * STATE), 1.0, 6.0, ((2, 4), (3, 8)), jnp.float32),
    }


EPS = 1e-05

def state_update(drive, active, current_rate, turn_now, size_now, in_pair, output_couple, skip_now, carried):
    sequences, positions = active.shape
    groups, entries = current_rate.shape
    members = in_pair.shape[-1]
    real_eig = -current_rate
    step_len = size_now[:, None]
    magnitude = jnp.exp(step_len * real_eig)
    decay_real = magnitude * jnp.cos(step_len * turn_now)
    decay_imag = magnitude * jnp.sin(step_len * turn_now)
    divisor = real_eig * real_eig + turn_now * turn_now
    hold_real = ((decay_real - 1.0) * real_eig + decay_imag * turn_now) / divisor
    hold_imag = (decay_imag * real_eig - (decay_real - 1.0) * turn_now) / divisor
    inject_real = hold_real[..., None] * in_pair[0] - hold_imag[..., None] * in_pair[1]
    inject_imag = hold_real[..., None] * in_pair[1] + hold_imag[..., None] * in_pair[0]
    inputs = drive.reshape(sequences, positions, groups, members)
    pushed_real = jnp.einsum('gpc,bsgc->bsgp', inject_real, inputs, precision=lax.Precision.HIGHEST)
    pushed_imag = jnp.einsum('gpc,bsgc->bsgp', inject_imag, inputs, precision=lax.Precision.HIGHEST)
    state_real_part = carried[0].reshape(sequences, groups, entries)
    state_imaginary = carried[1].reshape(sequences, groups, entries)
    readings = []
    for position in range(positions):
        active_now = (active[:, position] > 0)[:, None, None]
        moved_real = decay_real * state_real_part - decay_imag * state_imaginary + pushed_real[:, position]
        moved_imag = decay_real * state_imaginary + decay_imag * state_real_part + pushed_imag[:, position]
        state_real_part = jnp.where(active_now, moved_real, state_real_part)
        state_imaginary = jnp.where(active_now, moved_imag, state_imaginary)
        readout_value = jnp.einsum('sal,usl->usa', output_couple[0], state_real_part, precision=lax.Precision.HIGHEST) - jnp.einsum('sal,usl->usa', output_couple[1], state_imaginary, precision=lax.Precision.HIGHEST)
        readings.append(readout_value)
    readout = jnp.stack(readings, axis=1) + skip_now.reshape(groups, members) * inputs
    final = jnp.stack([state_real_part.reshape(sequences, groups * entries), state_imaginary.reshape(sequences, groups * entries)])
    return (readout.reshape(sequences * positions, groups * members), final)

def reference(tokens, lengths, norm_gains, drive_proj, open_proj, glu_proj, merge_proj, exit_proj, decay_rate, turn_rate, group_step_width, state_in, state_out, skip_gain, carried_state):
    sequences, positions, model_width = tokens.shape
    row_count = sequences * positions
    active = (lax.broadcasted_iota(jnp.int32, (sequences, positions), 1) < lengths[:, None]).astype(jnp.int32)
    active_rows = active.reshape(row_count, 1).astype(jnp.float32)
    residual = tokens.reshape(row_count, model_width)
    states = []
    for layer_index in range(LAYERS):
        values = residual.astype(jnp.float32)
        inverse_rms = lax.rsqrt(lax.optimization_barrier(jnp.mean(values * values, axis=1, keepdims=True)) + EPS)
        normed = (values * inverse_rms * norm_gains[layer_index]).astype(jnp.bfloat16)
        drive = jnp.dot(normed, drive_proj[layer_index], preferred_element_type=jnp.float32)
        gate_open = jax.nn.sigmoid(jnp.dot(normed, open_proj[layer_index], preferred_element_type=jnp.float32))
        readout, final = state_update(drive, active, decay_rate[layer_index], turn_rate[layer_index], group_step_width[layer_index], state_in[layer_index], state_out[layer_index], skip_gain[layer_index], carried_state[layer_index])
        states.append(final)
        activated = jax.nn.gelu(readout).astype(jnp.bfloat16)
        gating = jnp.dot(activated, glu_proj[layer_index], preferred_element_type=jnp.float32)
        gated = (activated.astype(jnp.float32) * jax.nn.sigmoid(gating)).astype(jnp.bfloat16)
        merged = jnp.dot(gated, merge_proj[layer_index], preferred_element_type=jnp.float32)
        mixed = (gate_open * merged).astype(jnp.bfloat16)
        branch = jnp.dot(mixed, exit_proj[layer_index], preferred_element_type=jnp.float32)
        residual = (residual.astype(jnp.float32) + active_rows * branch).astype(jnp.bfloat16)
    return (residual.reshape(sequences, positions, model_width), jnp.stack(states))
```

```python
import jax
import jax.numpy as jnp
from jax import lax
from jax.sharding import PartitionSpec as P

EPS = 1e-05


def state_update(
    drive, live, current_rate, turn_now, size_now, in_pair, output_couple, skip_now, carried
):
    positions, sequences, _ = live.shape
    groups, entries = current_rate.shape
    members = in_pair.shape[-1]
    real_eig = -current_rate
    step_len = size_now[:, None]
    magnitude = jnp.exp(step_len * real_eig)
    decay_real = magnitude * jnp.cos(step_len * turn_now)
    decay_imag = magnitude * jnp.sin(step_len * turn_now)
    divisor = real_eig * real_eig + turn_now * turn_now
    hold_real = ((decay_real - 1.0) * real_eig + decay_imag * turn_now) / divisor
    hold_imag = (decay_imag * real_eig - (decay_real - 1.0) * turn_now) / divisor
    width = groups * entries
    decay_real, decay_imag, hold_real, hold_imag = (
        value.reshape(1, width) for value in (decay_real, decay_imag, hold_real, hold_imag)
    )
    in_real, in_imag = (jnp.transpose(in_pair[i], (2, 0, 1)).reshape(members, width) for i in (0, 1))
    inject_real = hold_real * in_real - hold_imag * in_imag
    inject_imag = hold_real * in_imag + hold_imag * in_real
    shape = (groups * members, width)
    same_group = (
        lax.broadcasted_iota(jnp.int32, shape, 0) // members
        == lax.broadcasted_iota(jnp.int32, shape, 1) // entries
    )
    inject = jnp.concatenate(
        [jnp.where(same_group, jnp.tile(part, (groups, 1)), 0.0) for part in (inject_real, inject_imag)],
        axis=1,
    )
    out_real, out_imag = (
        jnp.where(
            same_group,
            jnp.tile(jnp.transpose(output_couple[i], (1, 0, 2)).reshape(members, width), (groups, 1)),
            0.0,
        )
        for i in (0, 1)
    )
    couple = jnp.concatenate([out_real, -out_imag], axis=1)
    pushed = jnp.dot(drive, inject, precision=lax.Precision.HIGHEST)
    state_real, state_imag = carried[0], carried[1]
    reached = []
    for position in range(positions):
        rows = pushed[position * sequences : (position + 1) * sequences]
        moved_real = decay_real * state_real - decay_imag * state_imag + rows[:, :width]
        moved_imag = decay_real * state_imag + decay_imag * state_real + rows[:, width:]
        state_real = jnp.where(live[position], moved_real, state_real)
        state_imag = jnp.where(live[position], moved_imag, state_imag)
        reached.append(jnp.concatenate([state_real, state_imag], axis=1))
    readout = lax.dot_general(
        jnp.concatenate(reached, axis=0),
        couple,
        (((1,), (1,)), ((), ())),
        precision=lax.Precision.HIGHEST,
    )
    return (readout + skip_now * drive, jnp.stack([state_real, state_imag]))


AXES = ("tp", "dp")
ROWS_PER_SEQUENCE = 3


def hypercube(values, bit):
    count = lax.axis_size("dp")
    return lax.ppermute(values, "dp", [(i, i ^ bit) for i in range(count)])


def rows_before(count):
    members = lax.axis_size("dp")
    me = lax.axis_index("dp")
    total = jnp.zeros_like(count)
    for shift in range(1, members):
        passed = lax.ppermute(count, "dp", [(i, i + shift) for i in range(members - shift)])
        total = total + passed
    return total


def pick_half(values, upper):
    half = values.shape[0] // 2
    return jnp.where(upper, values[half:], values[:half])


def both_halves(own, upper):
    other = hypercube(own, 1)
    return jnp.concatenate([jnp.where(upper, other, own), jnp.where(upper, own, other)], axis=0)


def reduce_half(partial, upper, wire):
    mine = pick_half(partial, upper)
    kept = mine.astype(jnp.float32) + hypercube(pick_half(partial, ~upper), 1).astype(jnp.float32)
    bit = 2
    while bit < lax.axis_size("dp"):
        kept = kept + hypercube(kept.astype(wire), bit).astype(jnp.float32)
        bit *= 2
    return kept


def spread(block):
    members, columns = lax.axis_size("dp"), lax.axis_size("tp")
    wide = columns // members
    line, across = lax.axis_index("tp") // wide, lax.axis_index("tp") % wide
    owner = lax.axis_index("dp")

    def at(d, z, x):
        return (z * wide + x) * members + d

    found = jnp.where(line == owner, block, jnp.zeros_like(block))
    for shift in range(1, members):
        perm = [
            (at(d, d, x), at(d, (d + shift) % members, x))
            for d in range(members)
            for x in range(wide)
        ]
        passed = lax.ppermute(block, AXES, perm)
        found = jnp.where(line == (owner + shift) % members, passed, found)
    pieces = [found]
    for flip in range(1, wide):
        perm = [(z * wide + x, z * wide + (x ^ flip)) for z in range(members) for x in range(wide)]
        pieces.append(lax.ppermute(found, "tp", perm))
    ordered = []
    for x in range(wide):
        piece = pieces[x]
        for mine in range(1, wide):
            piece = jnp.where(across == mine, pieces[x ^ mine], piece)
        ordered.append(piece)
    return jnp.concatenate(ordered, axis=1)


def project(gathered, weight):
    return jnp.dot(gathered, weight, preferred_element_type=jnp.float32)


def shards(
    tokens,
    lengths,
    norm_gains,
    drive_proj,
    open_proj,
    glu_proj,
    merge_proj,
    exit_proj,
    decay_rate,
    turn_rate,
    group_step_width,
    state_in,
    state_out,
    skip_gain,
    carried_state,
):
    sequences, positions, local_width = tokens.shape
    row_count = sequences * positions
    members = lax.axis_size("dp")
    model_width = local_width * lax.axis_size("tp")
    slice_width = model_width // members
    live_rows = ROWS_PER_SEQUENCE * sequences * members
    me = lax.axis_index("dp")
    upper = (me & 1) == 1
    slot = lax.broadcasted_iota(jnp.int32, (sequences, positions), 1)
    active = (slot < lengths[:, None]).astype(jnp.int32)
    earlier = lax.broadcasted_iota(jnp.int32, (sequences, sequences), 1) < lax.broadcasted_iota(
        jnp.int32, (sequences, sequences), 0
    )
    before = jnp.sum(jnp.where(earlier, lengths[None, :], 0), axis=1)
    start = rows_before(jnp.sum(lengths).reshape(1))
    place = jnp.where(active > 0, start + before[:, None] + slot, -1).reshape(1, row_count)
    placing = lax.broadcasted_iota(jnp.int32, (live_rows, row_count), 0) == place
    placing_bf = placing.astype(jnp.bfloat16)
    slot_major = lax.broadcasted_iota(jnp.int32, (positions, sequences), 0)
    live = slot_major < lengths[None, :]
    place_major = jnp.where(live, start + before[None, :] + slot_major, -1).reshape(1, row_count)
    placing_major = lax.broadcasted_iota(jnp.int32, (live_rows, row_count), 0) == place_major
    placing_f32 = placing_major.astype(jnp.float32)
    placing_major_bf = placing_major.astype(jnp.bfloat16)

    def compact(chosen, values):
        return jnp.dot(chosen, values, preferred_element_type=jnp.float32).astype(jnp.bfloat16)

    own_tokens = tokens.reshape(row_count, local_width)
    residual = reduce_half(compact(placing_bf, own_tokens), upper, jnp.bfloat16).astype(jnp.bfloat16)
    states = []
    for layer_index in range(norm_gains.shape[0]):
        own_gain = lax.dynamic_slice_in_dim(norm_gains[layer_index], me * slice_width, slice_width, 0)
        values = spread(both_halves(residual, upper)).astype(jnp.float32)
        squares = reduce_half(jnp.sum(values * values, axis=1), upper, jnp.float32)
        inverse_rms = lax.rsqrt(squares / model_width + EPS)[:, None]
        scaled = (values * own_gain).astype(jnp.bfloat16)
        drive_half = inverse_rms * reduce_half(
            project(scaled, drive_proj[layer_index]), upper, jnp.float32
        )
        drive = lax.dot_general(
            placing_f32,
            both_halves(drive_half, upper),
            (((0,), (0,)), ((), ())),
            precision=lax.Precision.HIGHEST,
        )
        gate_open = jax.nn.sigmoid(
            inverse_rms * reduce_half(project(scaled, open_proj[layer_index]), upper, jnp.bfloat16)
        )
        readout, final = state_update(
            drive,
            live[:, :, None],
            decay_rate[layer_index],
            turn_rate[layer_index],
            group_step_width[layer_index],
            state_in[layer_index],
            state_out[layer_index],
            skip_gain[layer_index],
            carried_state[layer_index],
        )
        states.append(final)
        activated = reduce_half(
            compact(placing_major_bf, jax.nn.gelu(readout).astype(jnp.bfloat16)), upper, jnp.bfloat16
        ).astype(jnp.bfloat16)
        gating = reduce_half(
            project(spread(both_halves(activated, upper)), glu_proj[layer_index]),
            upper,
            jnp.bfloat16,
        )
        gated = (activated.astype(jnp.float32) * jax.nn.sigmoid(gating)).astype(jnp.bfloat16)
        merged = reduce_half(
            project(spread(both_halves(gated, upper)), merge_proj[layer_index]),
            upper,
            jnp.bfloat16,
        )
        mixed = (gate_open * merged).astype(jnp.bfloat16)
        branch = reduce_half(
            project(spread(both_halves(mixed, upper)), exit_proj[layer_index]),
            upper,
            jnp.bfloat16,
        )
        residual = (residual.astype(jnp.float32) + branch).astype(jnp.bfloat16)
    moved = lax.dot_general(
        placing_bf,
        both_halves(residual, upper),
        (((0,), (0,)), ((), ())),
        preferred_element_type=jnp.float32,
    ).astype(jnp.bfloat16)
    updated = jnp.where(active.reshape(row_count, 1) > 0, moved, own_tokens)
    return (updated.reshape(sequences, positions, local_width), jnp.stack(states))


def solution(mesh):
    in_specs = (
        P("dp", None, "tp"),
        P("dp"),
        P(),
        P(None, "dp", "tp"),
        P(None, "dp", "tp"),
        P(None, "dp", "tp"),
        P(None, "dp", "tp"),
        P(None, "dp", "tp"),
        P(None, "tp", None),
        P(None, "tp", None),
        P(None, "tp"),
        P(None, None, "tp", None, None),
        P(None, None, "tp", None, None),
        P(None, "tp"),
        P(None, None, "dp", "tp"),
    )
    out_specs = (P("dp", None, "tp"), P(None, None, "dp", "tp"))
    return jax.shard_map(shards, mesh=mesh, in_specs=in_specs, out_specs=out_specs, check_vma=False)
```
